32 devices in a mesh: sp: 16 (over z, y, x), tp: 2 (over core).
Axes of the slice: x: 2, y: 2, z: 4, core: 2. Of those that a mesh axis runs over, the one named last changes fastest.
Arguments:
- query_proj: bfloat16 [4096, 1024], P('sp', 'tp'), may hold values from -6 to 6
- key_proj: bfloat16 [4096, 512], P('sp', 'tp'), may hold values from -6 to 6
- value_proj: bfloat16 [4096, 512], P('sp', 'tp'), may hold values from -6 to 6
- q_gain: float32 [64], replicated, may hold values from 1.1 to 10, as said below
- k_gain: float32 [64], replicated, may hold values from 1.1 to 10, as said below
- residual: bfloat16 [4096, 2048], P('sp'), may hold values from -6 to 6
- out_weight: bfloat16 [1024, 2048], P('tp'), may hold values from -0.75 to 0.75
- norm_gain: float32 [2048], replicated, may hold values from 0.1 to 1.9
- value_weight: bfloat16 [2048, 5120], P('sp', 'tp'), may hold values from -0.125 to 0.125
- gate_weight: bfloat16 [2048, 5120], P('sp', 'tp'), may hold values from -0.125 to 0.125
- down_weight: bfloat16 [5120, 2048], P('tp', 'sp'), may hold values from -0.078125 to 0.078125
- conv_value: float32 [3, 5120], P(None, 'tp'), may hold values from -3.5 to 3.5
- conv_gate: float32 [3, 5120], P(None, 'tp'), may hold values from -3.5 to 3.5
Outputs:
- layer_out: bfloat16 [4096, 2048], P(('sp', 'tp'))
The draws below stay inside these ranges and needn't reach their ends.
Inputs may be any that keep to these rules, and one draw needn't show every extreme that they name: `q_gain`: per-dimension gains of the query norm. `k_gain`: per-dimension gains of the key norm.
All inputs are finite; a program needn't handle non-finite values.
Results may differ from the reference program's by a relative error of at most 0.015.
The reference program's roundings to bfloat16 on the way count: a program that leaves them out, or rounds other values in their place, can miss the bound.
Values may be sent and summed in bfloat16 or wider, within the bound.
A program may use at most 128 MiB of HBM per device.

```python
import math
import jax
import jax.numpy as jnp
from jax import lax

D = 2048
HEADS = 16
KV_HEADS = 8
HEAD_DIM = 64
FF = 5120
GRID_W = 64
CONV_W = 3
SEQ = 4096
N_TP = 2


def gain_draw(key, salt_value):
    key_here = jax.random.fold_in(key, salt_value)
    return jnp.exp(jax.random.uniform(key_here, (HEAD_DIM,), jnp.float32, jnp.log(1.1), jnp.log(2.0)))


def draw_q_gain(key, part):
    return gain_draw(key, 11)


def draw_k_gain(key, part):
    return gain_draw(key, 23)


def block_scale(key, dims, pieces, least, top_value):
    gain, own = 1.0, jax.random.fold_in(key, 6)
    for axis_at, parts in pieces:
        steps = jnp.exp(jax.random.uniform(jax.random.fold_in(own, axis_at), (parts,), jnp.float32, least / len(pieces), top_value / len(pieces)))
        gain = gain * jnp.repeat(steps, dims[axis_at] // parts).reshape([-1 if axis == axis_at else 1 for axis in range(len(dims))])
    return gain


def centred(rng, extent, width, limit, cuts=(), kind=jnp.bfloat16):
    result = width * jax.random.normal(rng, extent, jnp.float32)
    if cuts:
        result = result * block_scale(rng, extent, cuts, -0.22, 0.18)
    return jnp.clip(result, -limit, limit).astype(kind)


def setup_inputs(seed: int = 0) -> dict:
    splits = jax.random.split(jax.random.key(seed), 14)
    query_proj = centred(splits[0], (SEQ, HEADS * HEAD_DIM), 1.0, 6.0, ((0, 16), (1, 2)))
    key_proj = centred(splits[1], (SEQ, KV_HEADS * HEAD_DIM), 1.0, 6.0, ((0, 16), (1, 2)))
    value_proj = centred(splits[2], (SEQ, KV_HEADS * HEAD_DIM), 1.0, 6.0, ((0, 16), (1, 2)))
    q_gain = draw_q_gain(jax.random.fold_in(splits[13], 71), 0)
    k_gain = draw_k_gain(jax.random.fold_in(splits[13], 71), 0)
    residual = centred(splits[5], (SEQ, D), 1.0, 6.0, ((0, 16),))
    out_weight = centred(splits[6], (HEADS * HEAD_DIM, D), (HEADS * HEAD_DIM // 16) ** -0.5, 0.75, ((0, 2),))
    norm_gain = jnp.clip(1.0 + 0.18 * jax.random.normal(splits[7], (D,), jnp.float32), 0.1, 1.9)
    value_weight = centred(splits[8], (D, FF), D ** -0.5, 0.125, ((0, 16), (1, 2)))
    gate_weight = centred(splits[9], (D, FF), D ** -0.5, 0.125, ((0, 16), (1, 2)))
    down_weight = centred(splits[10], (FF, D), FF ** -0.5, 0.078125, ((0, 2), (1, 16)))
    conv_value = centred(splits[11], (CONV_W, FF), CONV_W ** -0.5, 3.5, ((1, 2),), jnp.float32)
    conv_gate = centred(splits[12], (CONV_W, FF), CONV_W ** -0.5, 3.5, ((1, 2),), jnp.float32)
    return {"query_proj": query_proj, "key_proj": key_proj, "value_proj": value_proj, "q_gain": q_gain, "k_gain": k_gain, "residual": residual, "out_weight": out_weight, "norm_gain": norm_gain, "value_weight": value_weight, "gate_weight": gate_weight, "down_weight": down_weight, "conv_value": conv_value, "conv_gate": conv_gate}


NORM_EPS = 1e-06
ROPE_BASE = 10000.0

def rms_norm(block_in, gain_vec):
    values = block_in.astype(jnp.float32)
    inv_rms = lax.rsqrt(lax.optimization_barrier(jnp.mean(values * values, axis=-1, keepdims=True)) + NORM_EPS)
    return values * inv_rms * gain_vec.astype(jnp.float32)

def rotate_half(values, position):
    full_width = values.shape[-1]
    half_width = full_width // 2
    frequency = ROPE_BASE ** (-jnp.arange(0, full_width, 2, dtype=jnp.float32) / full_width)
    angles = position.astype(jnp.float32)[:, None] * frequency[None, :]
    cosine = jnp.cos(angles)[:, None, :]
    sine_part = jnp.sin(angles)[:, None, :]
    first_half = values[..., :half_width]
    second_half = values[..., half_width:]
    return jnp.concatenate([first_half * cosine - second_half * sine_part, first_half * sine_part + second_half * cosine], axis=-1)

def grid_rotary(values, positions):
    half_width = values.shape[-1] // 2
    grid_row = positions // GRID_W
    column = positions % GRID_W
    return jnp.concatenate([rotate_half(values[..., :half_width], grid_row), rotate_half(values[..., half_width:], column)], axis=-1)

def depthwise(up_rows, tap_weights):
    padded = jnp.pad(up_rows.astype(jnp.float32), ((1, 1), (0, 0)))
    weights = tap_weights.astype(jnp.float32)
    return padded[:-2] * weights[0] + padded[1:-1] * weights[1] + padded[2:] * weights[2]

def reference(query_proj, key_proj, value_proj, q_gain, k_gain, residual, out_weight, norm_gain, value_weight, gate_weight, down_weight, conv_value, conv_gate):
    sequence = query_proj.shape[0]
    positions = jnp.arange(sequence, dtype=jnp.int32)
    group_size = HEADS // KV_HEADS
    queries = grid_rotary(rms_norm(query_proj.reshape(sequence, HEADS, HEAD_DIM), q_gain), positions) * HEAD_DIM ** (-0.5)
    queries = lax.optimization_barrier(queries.astype(jnp.bfloat16)).astype(jnp.float32)
    keys_rot = grid_rotary(rms_norm(key_proj.reshape(sequence, KV_HEADS, HEAD_DIM), k_gain), positions)
    keys_rot = lax.optimization_barrier(keys_rot.astype(jnp.bfloat16)).astype(jnp.float32)
    keys_rep = jnp.repeat(keys_rot, group_size, axis=1)
    values_rep = jnp.repeat(value_proj.reshape(sequence, KV_HEADS, HEAD_DIM).astype(jnp.float32), group_size, axis=1)
    q_span = math.gcd(sequence, 256)

    def attend(q_block):
        scores = jnp.einsum('qhd,shd->hqs', q_block, keys_rep)
        row_max = lax.optimization_barrier(jnp.max(scores, axis=-1, keepdims=True))
        weights = jnp.exp(scores - row_max)
        totals = lax.optimization_barrier(jnp.sum(weights, axis=-1))
        rounded = lax.optimization_barrier(weights.astype(jnp.bfloat16)).astype(jnp.float32)
        summed = jnp.einsum('hqs,shd->qhd', rounded, values_rep)
        return summed / jnp.transpose(totals)[:, :, None]
    results = lax.map(attend, queries.reshape(sequence // q_span, q_span, HEADS, HEAD_DIM))
    attended = results.reshape(sequence, HEADS * HEAD_DIM).astype(jnp.bfloat16)
    head_cols = HEADS * HEAD_DIM // N_TP
    mix_sum = jnp.zeros((sequence, D), jnp.float32)
    for group_index in range(N_TP):
        partial_sum = jnp.dot(attended[:, group_index * head_cols:(group_index + 1) * head_cols], out_weight[group_index * head_cols:(group_index + 1) * head_cols], preferred_element_type=jnp.float32)
        mix_sum = mix_sum + lax.optimization_barrier(partial_sum.astype(jnp.bfloat16)).astype(jnp.float32)
    mix_out = mix_sum.astype(jnp.bfloat16)
    updated = (residual.astype(jnp.float32) + mix_out.astype(jnp.float32)).astype(jnp.bfloat16)
    normed = rms_norm(updated, norm_gain).astype(jnp.bfloat16)
    value_up = jnp.dot(normed, value_weight, preferred_element_type=jnp.float32).astype(jnp.bfloat16)
    gate_up = jnp.dot(normed, gate_weight, preferred_element_type=jnp.float32).astype(jnp.bfloat16)
    conv_val = depthwise(value_up, conv_value)
    conv_gated = depthwise(gate_up, conv_gate)
    hidden = (jax.nn.gelu(conv_gated, approximate=True) * conv_val).astype(jnp.bfloat16)
    ff_cols = FF // N_TP
    branch_sum = jnp.zeros((sequence, D), jnp.float32)
    for group_index in range(N_TP):
        partial_sum = jnp.dot(hidden[:, group_index * ff_cols:(group_index + 1) * ff_cols], down_weight[group_index * ff_cols:(group_index + 1) * ff_cols], preferred_element_type=jnp.float32)
        branch_sum = branch_sum + lax.optimization_barrier(partial_sum.astype(jnp.bfloat16)).astype(jnp.float32)
    branch = branch_sum.astype(jnp.bfloat16)
    return (updated.astype(jnp.float32) + branch.astype(jnp.float32)).astype(jnp.bfloat16)
```

```python
import functools
import math

import jax
import jax.numpy as jnp
from jax import lax
from jax.experimental import pallas as pl
from jax.sharding import PartitionSpec as P

HEAD_DIM = 64
GRID_W = 64


NORM_EPS = 1e-06
ROPE_BASE = 10000.0


def rms_norm(block_in, gain_vec):
    values = block_in.astype(jnp.float32)
    inv_rms = lax.rsqrt(jnp.mean(values * values, axis=-1, keepdims=True) + NORM_EPS)
    return values * inv_rms * gain_vec


def rotate_half(values, position):
    full_width = values.shape[-1]
    half_width = full_width // 2
    frequency = ROPE_BASE ** (-jnp.arange(0, full_width, 2, dtype=jnp.float32) / full_width)
    angles = position.astype(jnp.float32)[:, None] * frequency[None, :]
    cosine = jnp.cos(angles)[:, None, :]
    sine_part = jnp.sin(angles)[:, None, :]
    first_half = values[..., :half_width]
    second_half = values[..., half_width:]
    return jnp.concatenate(
        [
            first_half * cosine - second_half * sine_part,
            first_half * sine_part + second_half * cosine,
        ],
        axis=-1,
    )


def grid_rotary(values, positions):
    half_width = values.shape[-1] // 2
    grid_row = positions // GRID_W
    column = positions % GRID_W
    return jnp.concatenate(
        [
            rotate_half(values[..., :half_width], grid_row),
            rotate_half(values[..., half_width:], column),
        ],
        axis=-1,
    )


def exchange_pieces(blocks, place, count, stride, axis_size):
    received = [lax.dynamic_index_in_dim(blocks, place, 0, keepdims=False)]
    for hop in range(1, count):
        block = lax.dynamic_index_in_dim(blocks, (place + hop) % count, 0, keepdims=False)
        received.append(lax.ppermute(block, "sp", shifted(hop, count, stride, axis_size)))
    return received


def shifted(hop, count, stride, axis_size):
    pairs = []
    for source in range(axis_size):
        group, rest = source // stride, source % stride
        pairs.append((source, ((group + hop) % count) * stride + rest))
    return pairs


def spread(block, count, stride):
    pieces = [block]
    for flip in range(1, stride):
        pairs = [
            (group * stride + rest, group * stride + (rest ^ flip))
            for group in range(count)
            for rest in range(stride)
        ]
        pieces.append(lax.ppermute(block, "sp", pairs))
    return pieces


def swap_cores(block):
    return lax.ppermute(block, "tp", [(0, 1), (1, 0)])


def in_core_order(mine, other, core):
    first = jnp.where(core == 0, mine, other)
    second = jnp.where(core == 0, other, mine)
    return jnp.concatenate([first, second], axis=0)


def attention_kernel(q_ref, k_ref, vt_ref, out_ref, *, span):
    queries = q_ref[...]
    rows, width = queries.shape
    run_max = jnp.full((1, rows), -1e30, jnp.float32)
    run_sum = jnp.zeros((1, rows), jnp.float32)
    run_acc = jnp.zeros((width, rows), jnp.float32)
    for start in range(0, k_ref.shape[0], span):
        scores = lax.dot_general(
            k_ref[start : start + span, :],
            queries,
            (((1,), (1,)), ((), ())),
            preferred_element_type=jnp.float32,
        )
        new_max = jnp.maximum(run_max, jnp.max(scores, axis=0, keepdims=True))
        probs = jnp.exp(scores - new_max)
        shrink = jnp.exp(run_max - new_max)
        run_sum = run_sum * shrink + jnp.sum(probs, axis=0, keepdims=True)
        run_acc = run_acc * shrink + jnp.dot(
            vt_ref[:, start : start + span],
            probs.astype(jnp.bfloat16),
            preferred_element_type=jnp.float32,
        )
        run_max = new_max
    out_ref[...] = (run_acc / run_sum).T.astype(jnp.bfloat16)


def attend(queries, keys, values_t):
    total, width = queries.shape
    key_count = keys.shape[0]
    block = math.gcd(total, 256)
    return pl.pallas_call(
        functools.partial(attention_kernel, span=math.gcd(key_count, 1024)),
        grid=(total // block,),
        out_shape=jax.ShapeDtypeStruct((total, width), jnp.bfloat16),
        in_specs=[
            pl.BlockSpec((block, width), lambda i: (i, 0)),
            pl.BlockSpec((key_count, width), lambda i: (0, 0)),
            pl.BlockSpec((width, key_count), lambda i: (0, 0)),
        ],
        out_specs=pl.BlockSpec((block, width), lambda i: (i, 0)),
        cost_estimate=pl.CostEstimate(
            flops=16 * total * key_count * width,
            bytes_accessed=4 * (total + key_count) * width,
            transcendentals=total * key_count,
        ),
    )(queries, keys, values_t)


def shards(
    query_proj,
    key_proj,
    value_proj,
    q_gain,
    k_gain,
    residual,
    out_weight,
    norm_gain,
    value_weight,
    gate_weight,
    down_weight,
    conv_value,
    conv_gate,
):
    tokens = query_proj.shape[0]
    heads_here = query_proj.shape[1] // HEAD_DIM
    kv_here = key_proj.shape[1] // HEAD_DIM
    group_size = heads_here // kv_here
    sp_size, tp_size = lax.axis_size("sp"), lax.axis_size("tp")
    count = math.gcd(sp_size, 4)
    stride = sp_size // count
    me, core = lax.axis_index("sp"), lax.axis_index("tp")
    place, rest = me // stride, me % stride
    positions = me * tokens + jnp.arange(tokens, dtype=jnp.int32)

    queries = grid_rotary(
        rms_norm(query_proj.reshape(tokens, heads_here, HEAD_DIM), q_gain), positions
    ) * HEAD_DIM ** (-0.5)
    queries = queries.astype(jnp.bfloat16)
    keys_rot = grid_rotary(
        rms_norm(key_proj.reshape(tokens, kv_here, HEAD_DIM), k_gain), positions
    ).astype(jnp.bfloat16)
    values = value_proj.reshape(tokens, kv_here, HEAD_DIM)

    ff_here = value_weight.shape[1]
    depth_here = value_weight.shape[0]
    hidden_here = ff_here // count

    split_heads = count if kv_here % count == 0 else 1
    kv_each = kv_here // split_heads
    packed = jnp.concatenate(
        [queries.reshape(tokens, kv_here, group_size * HEAD_DIM), keys_rot, values], axis=2
    ).transpose(1, 0, 2)
    packed = packed.reshape(split_heads, kv_each, tokens, (group_size + 2) * HEAD_DIM)
    if split_heads > 1:
        got = exchange_pieces(packed, place, count, stride, sp_size)
        got, weights_in = lax.optimization_barrier((got, (value_weight, gate_weight, down_weight)))
    else:
        got, weights_in = [packed[0]], (value_weight, gate_weight, down_weight)
    value_in, gate_in, down_in = weights_in

    q_width = group_size * HEAD_DIM
    kv_mine = jnp.stack([piece[..., q_width:] for piece in got])
    if split_heads > 1:
        kv_all = jnp.stack(spread(kv_mine, count, stride))
    else:
        kv_all = lax.all_gather(kv_mine, "sp", axis=0)
    kv_all = kv_all.transpose(2 + 0, 0, 1, 3, 4).reshape(kv_each, sp_size * tokens, 2 * HEAD_DIM)

    up_blocks = jnp.concatenate(
        [
            value_in.reshape(depth_here, count, hidden_here),
            gate_in.reshape(depth_here, count, hidden_here),
        ],
        axis=2,
    ).transpose(1, 0, 2)
    up_rows = jnp.stack(exchange_pieces(up_blocks, place, count, stride, sp_size))
    up_rows = jnp.roll(up_rows[::-1], place + 1, axis=0)
    up_pieces = spread(up_rows.reshape(count * depth_here, 2 * hidden_here), count, stride)
    columns_here = down_weight.shape[1]
    down_blocks = down_in.reshape(count, hidden_here, columns_here)
    down_cols = jnp.stack(exchange_pieces(down_blocks, place, count, stride, sp_size))
    down_cols = jnp.roll(down_cols[::-1], place + 1, axis=0).transpose(1, 0, 2)
    down_pieces = spread(down_cols.reshape(hidden_here, count * columns_here), count, stride)

    q_pieces = [piece[..., :q_width] for piece in got]
    per_head = []
    for kv_at in range(kv_each):
        keys_h = kv_all[kv_at, :, :HEAD_DIM]
        values_t = kv_all[kv_at, :, HEAD_DIM:].T
        per_group = []
        for group_at in range(group_size):
            columns = slice(group_at * HEAD_DIM, (group_at + 1) * HEAD_DIM)
            q_here = jnp.concatenate([piece[kv_at, :, columns] for piece in q_pieces], axis=0)
            per_group.append(attend(q_here, keys_h, values_t))
        per_head.append(jnp.concatenate(per_group, axis=1))
    done = jnp.concatenate(per_head, axis=1).reshape(len(got), tokens, -1)
    if split_heads > 1:
        back = [done[0]]
        for hop in range(1, count):
            back.append(lax.ppermute(done[hop], "sp", shifted(-hop, count, stride, sp_size)))
        attended = jnp.roll(jnp.stack(back), place, axis=0).transpose(1, 0, 2)
        attended = attended.reshape(tokens, heads_here * HEAD_DIM)
    else:
        attended = done[0]

    row_share = tokens // tp_size
    residual_mine = lax.dynamic_slice_in_dim(residual, core * row_share, row_share, 0)
    if tp_size == 2:
        weight_other = swap_cores(out_weight)
        halves = attended.reshape(2, row_share, heads_here * HEAD_DIM)
        rows_mine = lax.dynamic_index_in_dim(halves, core, 0, keepdims=False)
        rows_other = swap_cores(lax.dynamic_index_in_dim(halves, 1 - core, 0, keepdims=False))
        mix_mine = jnp.dot(rows_mine, out_weight, preferred_element_type=jnp.float32)
        mix_other = jnp.dot(rows_other, weight_other, preferred_element_type=jnp.float32)
        mix_out = (
            mix_mine.astype(jnp.bfloat16).astype(jnp.float32)
            + mix_other.astype(jnp.bfloat16).astype(jnp.float32)
        ).astype(jnp.bfloat16)
    else:
        mix_out = lax.psum_scatter(
            jnp.dot(attended, out_weight, preferred_element_type=jnp.float32).astype(jnp.bfloat16),
            "tp",
            scatter_dimension=0,
            tiled=True,
        )
    updated = (residual_mine.astype(jnp.float32) + mix_out.astype(jnp.float32)).astype(jnp.bfloat16)
    normed = rms_norm(updated, norm_gain).astype(jnp.bfloat16)
    width = normed.shape[1]
    normed = normed.reshape(row_share, count, stride, depth_here).transpose(2, 0, 1, 3)
    normed = normed.reshape(stride, row_share, count * depth_here)

    ups = []
    for hop in range(count):
        rows = normed
        if hop:
            rows = lax.ppermute(normed, "sp", shifted(hop, count, stride, sp_size))
        if tp_size == 2:
            other = swap_cores(rows)
            rows = jnp.concatenate(
                [jnp.where(core == 0, rows, other), jnp.where(core == 0, other, rows)], axis=1
            )
        else:
            rows = lax.all_gather(rows, "tp", axis=1, tiled=True)
        total = 0.0
        for flip in range(stride):
            part = lax.dynamic_index_in_dim(rows, rest ^ flip, 0, keepdims=False)
            total = total + jnp.dot(part, up_pieces[flip], preferred_element_type=jnp.float32)
        ups.append(total.astype(jnp.bfloat16))
    ups = jnp.stack(ups)

    forward = [
        (group * stride + at, group * stride + (at + 1) % stride)
        for group in range(count)
        for at in range(stride)
    ]
    backward = [(target, source) for source, target in forward]
    before = lax.ppermute(ups[:, -1], "sp", forward)
    after = lax.ppermute(ups[:, 0], "sp", backward)
    hops = jnp.arange(count)
    block_at = (place - hops) % count
    no_before = (rest == 0) & (block_at == 0)
    no_after = (rest == stride - 1) & (block_at == count - 1)
    before = jnp.where(rest == 0, jnp.roll(before, -1, axis=0), before)
    after = jnp.where(rest == stride - 1, jnp.roll(after, 1, axis=0), after)
    before = jnp.where(no_before[:, None], 0, before)
    after = jnp.where(no_after[:, None], 0, after)
    padded = jnp.concatenate([before[:, None], ups, after[:, None]], axis=1).astype(jnp.float32)
    taps = jnp.concatenate(
        [
            lax.dynamic_slice_in_dim(conv_value, place * hidden_here, hidden_here, 1),
            lax.dynamic_slice_in_dim(conv_gate, place * hidden_here, hidden_here, 1),
        ],
        axis=1,
    )
    conv = padded[:, :-2] * taps[0] + padded[:, 1:-1] * taps[1] + padded[:, 2:] * taps[2]
    hidden = (
        jax.nn.gelu(conv[..., hidden_here:], approximate=True) * conv[..., :hidden_here]
    ).astype(jnp.bfloat16)

    down_all = jnp.concatenate(down_pieces, axis=1)
    branch = 0.0
    for hop in list(range(1, count)) + [0]:
        partial = jnp.dot(hidden[hop], down_all, preferred_element_type=jnp.float32)
        if tp_size == 2:
            partial = partial.reshape(2, row_share, width)
            mine = lax.dynamic_index_in_dim(partial, core, 0, keepdims=False)
            theirs = lax.dynamic_index_in_dim(partial, 1 - core, 0, keepdims=False)
            other = swap_cores(theirs.astype(jnp.bfloat16))
            mine = mine + other.astype(jnp.float32)
        else:
            mine = lax.psum_scatter(
                partial.astype(jnp.bfloat16), "tp", scatter_dimension=0, tiled=True
            )
        if hop:
            mine = lax.ppermute(
                mine.astype(jnp.bfloat16), "sp", shifted(-hop, count, stride, sp_size)
            )
        branch = branch + mine.astype(jnp.float32)
    branch = branch.astype(jnp.bfloat16).reshape(row_share, stride, count, columns_here)
    order = rest ^ jnp.arange(stride)
    branch = jnp.take(branch, order, axis=1).transpose(0, 2, 1, 3).reshape(row_share, width)
    return (updated.astype(jnp.float32) + branch.astype(jnp.float32)).astype(jnp.bfloat16)


def solution(mesh):
    return jax.shard_map(
        shards,
        mesh=mesh,
        in_specs=(
            P("sp", "tp"),
            P("sp", "tp"),
            P("sp", "tp"),
            P(),
            P(),
            P("sp", None),
            P("tp", None),
            P(),
            P("sp", "tp"),
            P("sp", "tp"),
            P("tp", "sp"),
            P(None, "tp"),
            P(None, "tp"),
        ),
        out_specs=P(("sp", "tp"), None),
        check_vma=False,
    )
```

```python
import functools
import math

import jax
import jax.numpy as jnp
from jax import lax
from jax.experimental import pallas as pl
from jax.sharding import PartitionSpec as P


HEAD_DIM = 64
GRID_W = 64


NORM_EPS = 1e-06
ROPE_BASE = 10000.0


def rms_norm(block_in, gain_vec):
    values = block_in.astype(jnp.float32)
    inv_rms = lax.rsqrt(jnp.mean(values * values, axis=-1, keepdims=True) + NORM_EPS)
    return values * inv_rms * gain_vec


def rotate_half(values, position):
    full_width = values.shape[-1]
    half_width = full_width // 2
    frequency = ROPE_BASE ** (-jnp.arange(0, full_width, 2, dtype=jnp.float32) / full_width)
    angles = position.astype(jnp.float32)[:, None] * frequency[None, :]
    cosine = jnp.cos(angles)[:, None, :]
    sine_part = jnp.sin(angles)[:, None, :]
    first_half = values[..., :half_width]
    second_half = values[..., half_width:]
    return jnp.concatenate(
        [
            first_half * cosine - second_half * sine_part,
            first_half * sine_part + second_half * cosine,
        ],
        axis=-1,
    )


def grid_rotary(values, positions):
    half_width = values.shape[-1] // 2
    grid_row = positions // GRID_W
    column = positions % GRID_W
    return jnp.concatenate(
        [
            rotate_half(values[..., :half_width], grid_row),
            rotate_half(values[..., half_width:], column),
        ],
        axis=-1,
    )


def exchange_pieces(block_for, place, count, stride, axis_size):
    received = [block_for(place)]
    for hop in range(1, count):
        block = block_for((place + hop) % count)
        received.append(lax.ppermute(block, "sp", shifted(hop, count, stride, axis_size)))
    return received


def in_place_order(received, place):
    count = len(received)
    doubled = (received[::-1] * 2)[: 2 * count - 1]
    size = received[0].shape[0]
    whole = jnp.concatenate(doubled, axis=0)
    return lax.dynamic_slice_in_dim(whole, (count - 1 - place) * size, count * size, 0)


def shifted(hop, count, stride, axis_size):
    pairs = []
    for source in range(axis_size):
        group, rest = source // stride, source % stride
        pairs.append((source, ((group + hop) % count) * stride + rest))
    return pairs


def spread(block, count, stride):
    pieces = [block]
    for flip in range(1, stride):
        pairs = [
            (group * stride + rest, group * stride + (rest ^ flip))
            for group in range(count)
            for rest in range(stride)
        ]
        pieces.append(lax.ppermute(block, "sp", pairs))
    return pieces


def unflip(pieces, rest):
    bit = 1
    while bit < len(pieces):
        chosen = (rest & bit) != 0
        pieces = [
            jnp.where(chosen, pieces[at ^ bit], pieces[at]) for at in range(len(pieces))
        ]
        bit *= 2
    return pieces


def swap_cores(block):
    return lax.ppermute(block, "tp", [(0, 1), (1, 0)])


def attention_kernel(q_ref, k_ref, vt_ref, out_ref, *, span):
    queries = q_ref[...]
    rows, width = queries.shape
    run_max = jnp.full((1, rows), -1e30, jnp.float32)
    run_sum = jnp.zeros((1, rows), jnp.float32)
    run_acc = jnp.zeros((width, rows), jnp.float32)
    for start in range(0, k_ref.shape[0], span):
        scores = lax.dot_general(
            k_ref[start : start + span, :],
            queries,
            (((1,), (1,)), ((), ())),
            preferred_element_type=jnp.float32,
        )
        new_max = jnp.maximum(run_max, jnp.max(scores, axis=0, keepdims=True))
        probs = jnp.exp(scores - new_max)
        shrink = jnp.exp(run_max - new_max)
        run_sum = run_sum * shrink + jnp.sum(probs, axis=0, keepdims=True)
        run_acc = run_acc * shrink + jnp.dot(
            vt_ref[:, start : start + span],
            probs.astype(jnp.bfloat16),
            preferred_element_type=jnp.float32,
        )
        run_max = new_max
    out_ref[...] = (run_acc / run_sum).T.astype(jnp.bfloat16)


def attend(queries, keys, values_t):
    total, width = queries.shape
    key_count = keys.shape[0]
    block = math.gcd(total, 256)
    return pl.pallas_call(
        functools.partial(attention_kernel, span=math.gcd(key_count, 1024)),
        grid=(total // block,),
        out_shape=jax.ShapeDtypeStruct((total, width), jnp.bfloat16),
        in_specs=[
            pl.BlockSpec((block, width), lambda i: (i, 0)),
            pl.BlockSpec((key_count, width), lambda i: (0, 0)),
            pl.BlockSpec((width, key_count), lambda i: (0, 0)),
        ],
        out_specs=pl.BlockSpec((block, width), lambda i: (i, 0)),
        cost_estimate=pl.CostEstimate(
            flops=16 * total * key_count * width,
            bytes_accessed=4 * (total + key_count) * width,
            transcendentals=total * key_count,
        ),
    )(queries, keys, values_t)


def shards(
    query_proj,
    key_proj,
    value_proj,
    q_gain,
    k_gain,
    residual,
    out_weight,
    norm_gain,
    value_weight,
    gate_weight,
    down_weight,
    conv_value,
    conv_gate,
):
    tokens = query_proj.shape[0]
    heads_here = query_proj.shape[1] // HEAD_DIM
    kv_here = key_proj.shape[1] // HEAD_DIM
    group_size = heads_here // kv_here
    sp_size, tp_size = lax.axis_size("sp"), lax.axis_size("tp")
    count = math.gcd(sp_size, 4)
    stride = sp_size // count
    me, core = lax.axis_index("sp"), lax.axis_index("tp")
    place, rest = me // stride, me % stride
    positions = me * tokens + jnp.arange(tokens, dtype=jnp.int32)

    queries = grid_rotary(
        rms_norm(query_proj.reshape(tokens, heads_here, HEAD_DIM), q_gain), positions
    ) * HEAD_DIM ** (-0.5)
    queries = queries.astype(jnp.bfloat16)
    keys_rot = grid_rotary(
        rms_norm(key_proj.reshape(tokens, kv_here, HEAD_DIM), k_gain), positions
    ).astype(jnp.bfloat16)
    values = value_proj.reshape(tokens, kv_here, HEAD_DIM)

    ff_here = value_weight.shape[1]
    depth_here = value_weight.shape[0]
    hidden_here = ff_here // count

    split_heads = count if kv_here % count == 0 else 1
    kv_each = kv_here // split_heads
    packed = jnp.concatenate(
        [queries.reshape(tokens, kv_here, group_size * HEAD_DIM), keys_rot, values], axis=2
    ).transpose(1, 0, 2)
    packed = packed.reshape(split_heads, kv_each, tokens, (group_size + 2) * HEAD_DIM)
    if split_heads > 1:
        got = exchange_pieces(
            lambda at: lax.dynamic_index_in_dim(packed, at, 0, keepdims=False),
            place,
            count,
            stride,
            sp_size,
        )
        got, weights_in = lax.optimization_barrier((got, (value_weight, gate_weight, down_weight)))
    else:
        got, weights_in = [packed[0]], (value_weight, gate_weight, down_weight)
    value_in, gate_in, down_in = weights_in

    q_width = group_size * HEAD_DIM
    kv_mine = jnp.stack([piece[..., q_width:] for piece in got])
    if split_heads > 1:
        kv_all = jnp.stack(spread(kv_mine, count, stride))
    else:
        kv_all = lax.all_gather(kv_mine, "sp", axis=0)
    kv_all = kv_all.transpose(2 + 0, 0, 1, 3, 4).reshape(kv_each, sp_size * tokens, 2 * HEAD_DIM)

    def up_block(at):
        start = at * hidden_here
        return jnp.concatenate(
            [
                lax.dynamic_slice_in_dim(value_in, start, hidden_here, 1),
                lax.dynamic_slice_in_dim(gate_in, start, hidden_here, 1),
            ],
            axis=1,
        )

    def down_block(at):
        return lax.dynamic_slice_in_dim(down_in, at * hidden_here, hidden_here, 0)

    up_got = exchange_pieces(up_block, place, count, stride, sp_size)
    up_pieces = spread(in_place_order(up_got, place), count, stride)
    columns_here = down_weight.shape[1]
    down_got = exchange_pieces(down_block, place, count, stride, sp_size)
    down_cols = in_place_order(down_got, place).reshape(count, hidden_here, columns_here)
    down_cols = jnp.concatenate([down_cols[at] for at in range(count)], axis=1)
    down_pieces = spread(down_cols, count, stride)

    q_pieces = [piece[..., :q_width] for piece in got]
    per_head = []
    for kv_at in range(kv_each):
        keys_h = kv_all[kv_at, :, :HEAD_DIM]
        values_t = kv_all[kv_at, :, HEAD_DIM:].T
        per_group = []
        for group_at in range(group_size):
            columns = slice(group_at * HEAD_DIM, (group_at + 1) * HEAD_DIM)
            q_here = jnp.concatenate([piece[kv_at, :, columns] for piece in q_pieces], axis=0)
            per_group.append(attend(q_here, keys_h, values_t))
        per_head.append(jnp.concatenate(per_group, axis=1))
    done = jnp.concatenate(per_head, axis=1).reshape(len(got), tokens, -1)
    if split_heads > 1:
        back = [done[0]]
        for hop in range(1, count):
            back.append(lax.ppermute(done[hop], "sp", shifted(-hop, count, stride, sp_size)))
        attended = jnp.roll(jnp.stack(back), place, axis=0).transpose(1, 0, 2)
        attended = attended.reshape(tokens, heads_here * HEAD_DIM)
    else:
        attended = done[0]

    row_share = tokens // tp_size
    residual_mine = lax.dynamic_slice_in_dim(residual, core * row_share, row_share, 0)
    if tp_size == 2:
        weight_other = swap_cores(out_weight)
        halves = attended.reshape(2, row_share, heads_here * HEAD_DIM)
        rows_mine = lax.dynamic_index_in_dim(halves, core, 0, keepdims=False)
        rows_other = swap_cores(lax.dynamic_index_in_dim(halves, 1 - core, 0, keepdims=False))
        mix_mine = jnp.dot(rows_mine, out_weight, preferred_element_type=jnp.float32)
        mix_other = jnp.dot(rows_other, weight_other, preferred_element_type=jnp.float32)
        mix_out = (
            mix_mine.astype(jnp.bfloat16).astype(jnp.float32)
            + mix_other.astype(jnp.bfloat16).astype(jnp.float32)
        ).astype(jnp.bfloat16)
    else:
        mix_out = lax.psum_scatter(
            jnp.dot(attended, out_weight, preferred_element_type=jnp.float32).astype(jnp.bfloat16),
            "tp",
            scatter_dimension=0,
            tiled=True,
        )
    updated = (residual_mine.astype(jnp.float32) + mix_out.astype(jnp.float32)).astype(jnp.bfloat16)
    normed = rms_norm(updated, norm_gain).astype(jnp.bfloat16)
    width = normed.shape[1]
    normed = jnp.stack(
        [
            jnp.concatenate(
                [
                    normed[:, (at * stride + flip) * depth_here :][:, :depth_here]
                    for at in range(count)
                ],
                axis=1,
            )
            for flip in range(stride)
        ]
    )

    ups = []
    for hop in range(count):
        rows = normed
        if hop:
            rows = lax.ppermute(normed, "sp", shifted(hop, count, stride, sp_size))
        if tp_size == 2:
            other = swap_cores(rows)
            rows = jnp.concatenate(
                [jnp.where(core == 0, rows, other), jnp.where(core == 0, other, rows)], axis=1
            )
        else:
            rows = lax.all_gather(rows, "tp", axis=1, tiled=True)
        total = 0.0
        for flip in range(stride):
            part = lax.dynamic_index_in_dim(rows, rest ^ flip, 0, keepdims=False)
            total = total + jnp.dot(part, up_pieces[flip], preferred_element_type=jnp.float32)
        ups.append(total.astype(jnp.bfloat16))
    ups = jnp.stack(ups)

    forward = [
        (group * stride + at, group * stride + (at + 1) % stride)
        for group in range(count)
        for at in range(stride)
    ]
    backward = [(target, source) for source, target in forward]
    before = lax.ppermute(ups[:, -1], "sp", forward)
    after = lax.ppermute(ups[:, 0], "sp", backward)
    hops = jnp.arange(count)
    block_at = (place - hops) % count
    no_before = (rest == 0) & (block_at == 0)
    no_after = (rest == stride - 1) & (block_at == count - 1)
    before = jnp.where(rest == 0, jnp.roll(before, -1, axis=0), before)
    after = jnp.where(rest == stride - 1, jnp.roll(after, 1, axis=0), after)
    before = jnp.where(no_before[:, None], 0, before)
    after = jnp.where(no_after[:, None], 0, after)
    padded = jnp.concatenate([before[:, None], ups, after[:, None]], axis=1).astype(jnp.float32)
    taps = jnp.concatenate(
        [
            lax.dynamic_slice_in_dim(conv_value, place * hidden_here, hidden_here, 1),
            lax.dynamic_slice_in_dim(conv_gate, place * hidden_here, hidden_here, 1),
        ],
        axis=1,
    )
    conv = padded[:, :-2] * taps[0] + padded[:, 1:-1] * taps[1] + padded[:, 2:] * taps[2]
    hidden = (
        jax.nn.gelu(conv[..., hidden_here:], approximate=True) * conv[..., :hidden_here]
    ).astype(jnp.bfloat16)

    down_all = jnp.concatenate(down_pieces, axis=1)
    branch = 0.0
    for hop in list(range(1, count)) + [0]:
        partial = jnp.dot(hidden[hop], down_all, preferred_element_type=jnp.float32)
        if tp_size == 2:
            partial = partial.reshape(2, row_share, width)
            mine = lax.dynamic_index_in_dim(partial, core, 0, keepdims=False)
            theirs = lax.dynamic_index_in_dim(partial, 1 - core, 0, keepdims=False)
            other = swap_cores(theirs.astype(jnp.bfloat16))
            mine = mine + other.astype(jnp.float32)
        else:
            mine = lax.psum_scatter(
                partial.astype(jnp.bfloat16), "tp", scatter_dimension=0, tiled=True
            )
        if hop:
            mine = lax.ppermute(
                mine.astype(jnp.bfloat16), "sp", shifted(-hop, count, stride, sp_size)
            )
        branch = branch + mine.astype(jnp.float32)
    branch = branch.astype(jnp.bfloat16)
    span = count * columns_here
    pieces = unflip([branch[:, at * span : (at + 1) * span] for at in range(stride)], rest)
    branch = jnp.concatenate(
        [
            pieces[at][:, group * columns_here : (group + 1) * columns_here]
            for group in range(count)
            for at in range(stride)
        ],
        axis=1,
    )
    return (updated.astype(jnp.float32) + branch.astype(jnp.float32)).astype(jnp.bfloat16)


def solution(mesh):
    return jax.shard_map(
        shards,
        mesh=mesh,
        in_specs=(
            P("sp", "tp"),
            P("sp", "tp"),
            P("sp", "tp"),
            P(),
            P(),
            P("sp", None),
            P("tp", None),
            P(),
            P("sp", "tp"),
            P("sp", "tp"),
            P("tp", "sp"),
            P(None, "tp"),
            P(None, "tp"),
        ),
        out_specs=P(("sp", "tp"), None),
        check_vma=False,
    )
```
